32 devices in a mesh: row: 8 (over z, y), col: 4 (over x, core).
Axes of the slice: x: 2, y: 2, z: 4, core: 2. Of those that a mesh axis runs over, the one named last changes fastest.
Arguments:
- tokens: bfloat16 [16384, 2048], P(('row', 'col')), may hold values from -6 to 6
- w_mix: bfloat16 [2048, 512], replicated, may hold values from -0.125 to 0.125
- w_gate: bfloat16 [2048, 2048], replicated, may hold values from -0.125 to 0.125
- gate_bias: float32 [2048], replicated, may hold values from -4 to 4
- w_branch: bfloat16 [512, 2048], replicated, may hold values from -0.25 to 0.25
Outputs:
- mixed: bfloat16 [16384, 2048], P(('row', 'col'))
The draws below stay inside these ranges and needn't reach their ends.
All inputs are finite; a program needn't handle non-finite values.
Results may differ from the reference program's by a relative error of at most 0.0083.
Values may be sent and summed in bfloat16 or wider, within the bound.
A program may use at most 64 MiB of HBM per device.

```python
import jax
import jax.numpy as jnp

D = 2048
FT_GROUPS = 8
GROUP_DIM = 64
FTW = 512
LENGTH = 16384


def block_scale(own_key, dims, split, smallest, largest):
    level, own = 1.0, jax.random.fold_in(own_key, 6)
    for dim, blocks in split:
        heights = jnp.exp(jax.random.uniform(jax.random.fold_in(own, dim), (blocks,), jnp.float32, smallest / len(split), largest / len(split)))
        level = level * jnp.repeat(heights, dims[dim] // blocks).reshape([-1 if axis == dim else 1 for axis in range(len(dims))])
    return level


def scatter_about(own_key, shape, spread, bound, pieces=(), dtype=jnp.bfloat16):
    gain = block_scale(own_key, shape, pieces, -0.22, 0.18) if pieces else 1.0
    entries = jax.random.normal(own_key, shape, jnp.float32) * spread * gain
    return jnp.minimum(jnp.maximum(entries, -bound), bound).astype(dtype)


def setup_inputs(seed: int = 0) -> dict:
    arg_keys = jax.random.split(jax.random.key(seed), 6)
    return {
        "tokens": scatter_about(arg_keys[0], (LENGTH, D), 1.0, 6.0, ((0, 32),)),
        "w_mix": scatter_about(arg_keys[1], (D, FTW), D ** -0.5, 0.125),
        "w_gate": scatter_about(arg_keys[2], (D, D), D ** -0.5, 0.125),
        "gate_bias": scatter_about(arg_keys[3], (D,), 1.0, 4.0, (), jnp.float32),
        "w_branch": scatter_about(arg_keys[4], (FTW, D), FTW ** -0.5, 0.25),
    }


def reference(tokens, w_mix, w_gate, gate_bias, w_branch):
    mixed_in = jnp.dot(tokens, w_mix, preferred_element_type=jnp.float32).astype(jnp.bfloat16)
    grouped = mixed_in.astype(jnp.float32).reshape(LENGTH, FT_GROUPS, GROUP_DIM)
    spectrum = jnp.fft.fft2(grouped, axes=(0, 2), norm="ortho").real
    spectrum = spectrum.reshape(LENGTH, FT_GROUPS * GROUP_DIM).astype(jnp.bfloat16)
    gate = jax.nn.sigmoid(jnp.dot(tokens, w_gate, preferred_element_type=jnp.float32) + gate_bias)
    branch = jnp.dot(spectrum, w_branch, preferred_element_type=jnp.float32)
    return (gate * branch).astype(jnp.bfloat16)
```

```python
import functools
import math

import jax
import jax.numpy as jnp
import numpy as np
from jax import lax
from jax.experimental import pallas as pl
from jax.experimental.pallas import tpu as pltpu
from jax.sharding import PartitionSpec as P

GROUP_DIM = 64
HALF = GROUP_DIM // 2
UNIT = 16
ROWS = 8
BLOCK = 128
SPAN = 256
MESH = pl.DeviceIdType.MESH


def phases(left, right, period):
    angle = (left[:, None] * right[None, :] % period) * (2.0 * math.pi / period)
    return np.cos(angle), np.sin(angle)


def channel_tables(span):
    index = np.arange(GROUP_DIM)
    packed = np.where(index <= HALF, index, index - HALF)
    cos_c, sin_c = phases(packed, index, GROUP_DIM)
    is_sin = index > HALF
    forward = np.where(is_sin[:, None], sin_c, cos_c)
    back = np.zeros((GROUP_DIM, GROUP_DIM))
    for row in index:
        freq = packed[row]
        mirror = (GROUP_DIM - freq) % GROUP_DIM
        back[row, freq] += -1.0 if is_sin[row] else 1.0
        if mirror != freq:
            back[row, mirror] += 1.0
    copies = np.eye(span // GROUP_DIM)
    return np.kron(copies, forward).astype(jnp.bfloat16), np.kron(copies, back).astype(jnp.bfloat16)


def plain(tokens, w_mix, w_gate, gate_bias, w_branch):
    axes = ("row", "col")
    n_dev = lax.axis_size(axes)
    local_len, full_len = tokens.shape[0], tokens.shape[0] * n_dev
    sub_len = local_len // n_dev
    channels = w_mix.shape[1]
    cols = channels // n_dev
    forward, back = channel_tables(channels)
    mixed_in = jnp.dot(tokens, w_mix, preferred_element_type=jnp.float32).astype(jnp.bfloat16)
    packed = jnp.einsum("ab,nb->an", forward, mixed_in, preferred_element_type=jnp.float32)
    packed = packed.astype(jnp.bfloat16).reshape(n_dev, cols, local_len)
    packed = lax.all_to_all(packed, axes, split_axis=0, concat_axis=0, tiled=True)
    dev, pos = np.arange(n_dev), np.arange(local_len)
    cos_p, sin_p = (t.astype(jnp.bfloat16) for t in phases(dev, dev, n_dev))
    cos_t, sin_t = (jnp.asarray(t, jnp.float32)[:, None, :] for t in phases(dev, pos, full_len))
    cos_m, sin_m = (t.astype(jnp.bfloat16) for t in phases(pos, pos, local_len))
    first_re = jnp.einsum("kp,pcj->kcj", cos_p, packed, preferred_element_type=jnp.float32)
    first_im = -jnp.einsum("kp,pcj->kcj", sin_p, packed, preferred_element_type=jnp.float32)
    column = lax.axis_index(axes) * cols + jnp.arange(cols, dtype=jnp.int32)
    is_sin = (column % GROUP_DIM > HALF)[None, :, None]
    rot_c, rot_s = jnp.where(is_sin, sin_t, cos_t), jnp.where(is_sin, -cos_t, sin_t)
    part_re = (first_re * rot_c + first_im * rot_s).astype(jnp.bfloat16)
    part_im = (first_im * rot_c - first_re * rot_s).astype(jnp.bfloat16)
    real = jnp.einsum("kcj,jm->kcm", part_re, cos_m, preferred_element_type=jnp.float32)
    real = real + jnp.einsum("kcj,jm->kcm", part_im, sin_m, preferred_element_type=jnp.float32)
    real = (real * (1.0 / math.sqrt(full_len * GROUP_DIM))).astype(jnp.bfloat16)
    real = real.reshape(n_dev, cols, n_dev, sub_len).transpose(2, 1, 0, 3)
    real = lax.all_to_all(real, axes, split_axis=0, concat_axis=0, tiled=True)
    rows = real.transpose(3, 2, 0, 1).reshape(local_len, channels)
    turned = jnp.dot(back, w_branch, preferred_element_type=jnp.float32).astype(jnp.bfloat16)
    gate = jax.nn.sigmoid(jnp.dot(tokens, w_gate, preferred_element_type=jnp.float32) + gate_bias)
    return (gate * jnp.dot(rows, turned, preferred_element_type=jnp.float32)).astype(jnp.bfloat16)


def dot(a, b):
    return jnp.dot(a, b, preferred_element_type=jnp.float32)


def dot_t(a, b):
    return lax.dot_general(a, b, (((1,), (1,)), ((), ())), preferred_element_type=jnp.float32)


def swap_units(block):
    units = [block[ROWS * i : ROWS * (i + 1)] for i in range(BLOCK // UNIT)]
    lane = lax.broadcasted_iota(jnp.int32, (ROWS, BLOCK), 1) // UNIT
    for bit in range(3):
        step = 1 << bit
        low = (lane // step) % 2 == 0
        for i in range(len(units)):
            if i & step:
                continue
            a, b = units[i], units[i + step]
            units[i] = jnp.where(low, a, pltpu.roll(b, UNIT * step, 1))
            units[i + step] = jnp.where(low, pltpu.roll(a, BLOCK - UNIT * step, 1), b)
    return units


def kernel(
    n, n_col, scale,
    tok_hbm, wmix_hbm, wgate_hbm, bias_hbm, wbr_hbm,
    fwd_hbm, back_hbm, first_hbm, cos_hbm, sin_hbm, last_hbm, perm_hbm,
    gate, partial, turned_b, rows_b,
    tok, wmix, wgate, bias_ref, wbr, fwd, back, first, cos_t, sin_t, last, perm,
    mixed, turned_a, rows_a,
    send1, recv1, send2, recv2,
    load_sem, s1_sem, r1_sem, s2_sem, r2_sem,
):
    me = lax.axis_index("row") * n_col + lax.axis_index("col")
    local_len, width = tok.shape
    channels = mixed.shape[1]
    half_len = local_len // 2

    pairs = (
        (wmix_hbm.at[:, pl.ds(0, SPAN)], wmix.at[0]),
        (tok_hbm.at[pl.ds(0, half_len)], tok.at[pl.ds(0, half_len)]),
        (tok_hbm.at[pl.ds(half_len, half_len)], tok.at[pl.ds(half_len, half_len)]),
        (fwd_hbm, fwd), (wmix_hbm.at[:, pl.ds(SPAN, SPAN)], wmix.at[1]),
        (bias_hbm, bias_ref), (wgate_hbm, wgate),
        (first_hbm, first), (cos_hbm, cos_t), (sin_hbm, sin_t), (last_hbm, last),
        (wbr_hbm, wbr), (back_hbm, back), (perm_hbm, perm),
    )
    loads = [pltpu.make_async_copy(a, b, load_sem.at[i]) for i, (a, b) in enumerate(pairs)]
    for i in range(5):
        loads[i].start()

    barrier = pltpu.get_barrier_semaphore()

    def greet(r, carry):
        peer = (me + r) % n
        pl.semaphore_signal(barrier, inc=1, device_id=(peer // n_col, peer % n_col), device_id_type=MESH)
        return carry

    lax.fori_loop(1, n, greet, 0)

    def remote(src, dst, s_sem, r_sem, h, peer, slot):
        return pltpu.make_async_remote_copy(
            src_ref=src.at[h, peer], dst_ref=dst.at[h, slot],
            send_sem=s_sem.at[h, peer], recv_sem=r_sem.at[h, slot],
            device_id=(peer // n_col, peer % n_col), device_id_type=MESH,
        )

    def each_peer(act):
        def step(r, carry):
            act((me + r) % n)
            return carry

        lax.fori_loop(1, n, step, 0)

    def own(src, dst, s_sem, r_sem, h):
        return pltpu.make_async_copy(src.at[h, me], dst.at[h, me], r_sem.at[h, me])

    def exchange(ex, h):
        each_peer(lambda peer: remote(*ex, h, peer, me).start())
        own(*ex, h).start()

    def arrived(ex, h):
        each_peer(lambda peer: remote(*ex, h, peer, peer).wait_recv())
        own(*ex, h).wait()

    def sent(ex, h):
        each_peer(lambda peer: remote(*ex, h, peer, me).wait_send())

    one = (send1, recv1, s1_sem, r1_sem)
    two = (send2, recv2, s2_sem, r2_sem)

    def pack(h):
        packed = dot_t(fwd[...], mixed[:, SPAN * h : SPAN * (h + 1)])
        send1[h] = packed.reshape(n, ROWS, local_len).astype(jnp.bfloat16)

    loads[0].wait()
    for i in range(2):
        at = slice(half_len * i, half_len * (i + 1))
        loads[1 + i].wait()
        mixed[at, :SPAN] = dot(tok[at, :], wmix[0]).astype(jnp.bfloat16)
    loads[3].wait()
    pack(0)
    pl.semaphore_wait(barrier, n - 1)
    exchange(one, 0)

    for i in range(5, len(loads)):
        loads[i].start()
    loads[4].wait()
    for i in range(2):
        at = slice(half_len * i, half_len * (i + 1))
        mixed[at, SPAN:] = dot(tok[at, :], wmix[1]).astype(jnp.bfloat16)
    pack(1)
    exchange(one, 1)

    loads[5].wait()
    loads[6].wait()

    def open_gate(i, carry):
        at = pl.ds(pl.multiple_of(i * SPAN, SPAN), SPAN)
        gate[:, at] = jax.nn.sigmoid(dot(tok[...], wgate[:, at]) + bias_ref[:, at])
        return carry

    lax.fori_loop(0, width // SPAN, open_gate, 0)
    for i in range(7, len(loads)):
        loads[i].wait()

    chunk = n * ROWS
    per = BLOCK // UNIT
    blocks = n // per

    def matrix(block):
        return block.astype(jnp.float32).reshape(chunk, local_len).astype(jnp.bfloat16)

    def turn(h, out):
        def step(j, carry):
            lanes = pl.ds(pl.multiple_of(j * SPAN, SPAN), SPAN)
            out[:, lanes] = dot(back[...], wbr[SPAN * h : SPAN * (h + 1), lanes]).astype(jnp.bfloat16)
            return carry

        lax.fori_loop(0, width // SPAN, step, 0)

    for h in range(2):
        column = h * chunk + me * ROWS + lax.broadcasted_iota(jnp.int32, (1, ROWS, local_len), 1)
        is_sin = column % GROUP_DIM > HALF
        arrived(one, h)
        gathered = matrix(recv1[h])
        first_re = dot(first[:chunk, :], gathered).reshape(n, ROWS, local_len)
        first_im = dot(first[chunk:, :], gathered).reshape(n, ROWS, local_len)
        c = jnp.broadcast_to(cos_t[...].reshape(n, 1, local_len), (n, ROWS, local_len))
        s = jnp.broadcast_to(sin_t[...].reshape(n, 1, local_len), (n, ROWS, local_len))
        c, s = jnp.where(is_sin, s, c), jnp.where(is_sin, -c, s)
        part_re = (first_re * c + first_im * s).reshape(chunk, local_len).astype(jnp.bfloat16)
        part_im = (first_im * c - first_re * s).reshape(chunk, local_len).astype(jnp.bfloat16)
        real = (dot(part_re, last[:local_len, :]) + dot(part_im, last[local_len:, :])) * scale
        for a in range(blocks):
            for b in range(blocks):
                block = real[ROWS * per * a : ROWS * per * (a + 1), BLOCK * b : BLOCK * (b + 1)]
                for i, unit in enumerate(swap_units(block)):
                    send2[h, per * b + i, :, BLOCK * a : BLOCK * (a + 1)] = unit.astype(jnp.bfloat16)
        exchange(two, h)
        if h == 0:
            turn(0, turned_a)

    turn(1, turned_b)
    sent(one, 0)
    sent(one, 1)
    arrived(two, 0)
    rows_a[...] = dot_t(perm[...], matrix(recv2[0])).astype(jnp.bfloat16)

    def first_half(j, carry):
        lanes = pl.ds(pl.multiple_of(j * SPAN, SPAN), SPAN)
        partial[:, lanes] = gate[:, lanes] * dot(rows_a[...], turned_a[:, lanes])
        return carry

    lax.fori_loop(0, width // SPAN, first_half, 0)
    sent(two, 0)
    arrived(two, 1)
    rows_b[...] = dot_t(perm[...], matrix(recv2[1])).astype(jnp.bfloat16)
    sent(two, 1)


def fused(tokens, w_mix, w_gate, gate_bias, w_branch):
    axes = ("row", "col")
    n_dev = lax.axis_size(axes)
    n_col = lax.axis_size("col")
    local_len, width = tokens.shape
    channels = w_mix.shape[1]
    full_len = local_len * n_dev
    bf16, f32 = jnp.bfloat16, jnp.float32

    dev, pos = np.arange(n_dev), np.arange(local_len)
    forward, back = channel_tables(SPAN)
    cos_p, sin_p = phases(dev, dev, n_dev)
    unit = np.eye(ROWS)
    first = np.concatenate([np.kron(cos_p, unit), np.kron(-sin_p, unit)]).astype(bf16)
    cos_t, sin_t = (t.astype(np.float32) for t in phases(dev, pos, full_len))
    last = np.concatenate(phases(pos, pos, local_len)).astype(bf16)
    order = (pos % n_dev) * UNIT + pos // n_dev
    perm = np.eye(local_len)[order].astype(bf16)

    tables = [forward, back, first, cos_t, sin_t, last, perm]
    any_space = pl.BlockSpec(memory_space=pl.ANY)
    block = pltpu.VMEM((2, n_dev, ROWS, local_len), bf16)
    sems = pltpu.SemaphoreType.DMA((2, n_dev))
    vmem = lambda array: pltpu.VMEM(array.shape, array.dtype)
    gate, partial, turned, rows = pl.pallas_call(
        functools.partial(kernel, n_dev, n_col, 1.0 / math.sqrt(full_len * GROUP_DIM)),
        out_shape=[
            pltpu.VMEM((local_len, width), f32),
            pltpu.VMEM((local_len, width), f32),
            pltpu.VMEM((SPAN, width), bf16),
            pltpu.VMEM((local_len, SPAN), bf16),
        ],
        in_specs=[any_space] * 12,
        out_specs=[pl.BlockSpec(memory_space=pltpu.VMEM)] * 4,
        scratch_shapes=[
            vmem(tokens), pltpu.VMEM((2, width, SPAN), bf16), vmem(w_gate), pltpu.VMEM((1, width), f32), vmem(w_branch),
            vmem(forward), vmem(back), vmem(first), vmem(cos_t), vmem(sin_t), vmem(last), vmem(perm),
            pltpu.VMEM((local_len, channels), bf16),
            pltpu.VMEM((SPAN, width), bf16),
            pltpu.VMEM((local_len, SPAN), bf16),
            block, block, block, block,
            pltpu.SemaphoreType.DMA((14,)),
            sems, sems, sems, sems,
        ],
        compiler_params=pltpu.CompilerParams(
            collective_id=0, has_side_effects=True, vmem_limit_bytes=57_200_000
        ),
    )(tokens, w_mix, w_gate, gate_bias.reshape(1, width), w_branch, *[jnp.asarray(t) for t in tables])
    return (partial + gate * dot(rows, turned)).astype(bf16)


def shards(tokens, w_mix, w_gate, gate_bias, w_branch):
    n_dev = lax.axis_size(("row", "col"))
    local_len, channels = tokens.shape[0], w_mix.shape[1]
    tiled = n_dev * ROWS == SPAN and channels == 2 * SPAN and local_len == n_dev * UNIT
    step = fused if tiled else plain
    return step(tokens, w_mix, w_gate, gate_bias, w_branch)


def solution(mesh):
    in_specs = (P(("row", "col"), None), P(), P(), P(), P())
    out_specs = P(("row", "col"), None)
    return jax.shard_map(shards, mesh=mesh, in_specs=in_specs, out_specs=out_specs, check_vma=False)
```

```python
import functools
import math

import jax
import jax.numpy as jnp
import numpy as np
from jax import lax
from jax.experimental import pallas as pl
from jax.experimental.pallas import tpu as pltpu
from jax.sharding import PartitionSpec as P

GROUP_DIM = 64
HALF = GROUP_DIM // 2
UNIT = 16
ROWS = 8
BLOCK = 128
SPAN = 256
MESH = pl.DeviceIdType.MESH


def phases(left, right, period):
    angle = (left[:, None] * right[None, :] % period) * (2.0 * math.pi / period)
    return np.cos(angle), np.sin(angle)


def channel_tables(span):
    index = np.arange(GROUP_DIM)
    packed = np.where(index <= HALF, index, index - HALF)
    cos_c, sin_c = phases(packed, index, GROUP_DIM)
    is_sin = index > HALF
    forward = np.where(is_sin[:, None], sin_c, cos_c)
    back = np.zeros((GROUP_DIM, GROUP_DIM))
    for row in index:
        freq = packed[row]
        mirror = (GROUP_DIM - freq) % GROUP_DIM
        back[row, freq] += -1.0 if is_sin[row] else 1.0
        if mirror != freq:
            back[row, mirror] += 1.0
    copies = np.eye(span // GROUP_DIM)
    return np.kron(copies, forward).astype(jnp.bfloat16), np.kron(copies, back).astype(jnp.bfloat16)


def plain(tokens, w_mix, w_gate, gate_bias, w_branch):
    axes = ("row", "col")
    n_dev = lax.axis_size(axes)
    local_len, full_len = tokens.shape[0], tokens.shape[0] * n_dev
    sub_len = local_len // n_dev
    channels = w_mix.shape[1]
    cols = channels // n_dev
    forward, back = channel_tables(channels)
    mixed_in = jnp.dot(tokens, w_mix, preferred_element_type=jnp.float32).astype(jnp.bfloat16)
    packed = jnp.einsum("ab,nb->an", forward, mixed_in, preferred_element_type=jnp.float32)
    packed = packed.astype(jnp.bfloat16).reshape(n_dev, cols, local_len)
    packed = lax.all_to_all(packed, axes, split_axis=0, concat_axis=0, tiled=True)
    dev, pos = np.arange(n_dev), np.arange(local_len)
    cos_p, sin_p = (t.astype(jnp.bfloat16) for t in phases(dev, dev, n_dev))
    cos_t, sin_t = (jnp.asarray(t, jnp.float32)[:, None, :] for t in phases(dev, pos, full_len))
    cos_m, sin_m = (t.astype(jnp.bfloat16) for t in phases(pos, pos, local_len))
    first_re = jnp.einsum("kp,pcj->kcj", cos_p, packed, preferred_element_type=jnp.float32)
    first_im = -jnp.einsum("kp,pcj->kcj", sin_p, packed, preferred_element_type=jnp.float32)
    column = lax.axis_index(axes) * cols + jnp.arange(cols, dtype=jnp.int32)
    is_sin = (column % GROUP_DIM > HALF)[None, :, None]
    rot_c, rot_s = jnp.where(is_sin, sin_t, cos_t), jnp.where(is_sin, -cos_t, sin_t)
    part_re = (first_re * rot_c + first_im * rot_s).astype(jnp.bfloat16)
    part_im = (first_im * rot_c - first_re * rot_s).astype(jnp.bfloat16)
    real = jnp.einsum("kcj,jm->kcm", part_re, cos_m, preferred_element_type=jnp.float32)
    real = real + jnp.einsum("kcj,jm->kcm", part_im, sin_m, preferred_element_type=jnp.float32)
    real = (real * (1.0 / math.sqrt(full_len * GROUP_DIM))).astype(jnp.bfloat16)
    real = real.reshape(n_dev, cols, n_dev, sub_len).transpose(2, 1, 0, 3)
    real = lax.all_to_all(real, axes, split_axis=0, concat_axis=0, tiled=True)
    rows = real.transpose(3, 2, 0, 1).reshape(local_len, channels)
    turned = jnp.dot(back, w_branch, preferred_element_type=jnp.float32).astype(jnp.bfloat16)
    gate = jax.nn.sigmoid(jnp.dot(tokens, w_gate, preferred_element_type=jnp.float32) + gate_bias)
    return (gate * jnp.dot(rows, turned, preferred_element_type=jnp.float32)).astype(jnp.bfloat16)


def dot(a, b):
    return jnp.dot(a, b, preferred_element_type=jnp.float32)


def dot_t(a, b):
    return lax.dot_general(a, b, (((1,), (1,)), ((), ())), preferred_element_type=jnp.float32)


def swap_units(block):
    units = [block[ROWS * i : ROWS * (i + 1)] for i in range(BLOCK // UNIT)]
    lane = lax.broadcasted_iota(jnp.int32, (ROWS, BLOCK), 1) // UNIT
    for bit in range(3):
        step = 1 << bit
        low = (lane // step) % 2 == 0
        for i in range(len(units)):
            if i & step:
                continue
            a, b = units[i], units[i + step]
            units[i] = jnp.where(low, a, pltpu.roll(b, UNIT * step, 1))
            units[i + step] = jnp.where(low, pltpu.roll(a, BLOCK - UNIT * step, 1), b)
    return units


def kernel(
    n, n_col, scale,
    tok_hbm, wmix_hbm, wgate_hbm, bias_hbm, wbr_hbm,
    fwd_hbm, back_hbm, first_hbm, cos_hbm, sin_hbm, last_hbm, perm_hbm,
    gate, partial, turned_b, rows_b,
    tok, wmix, wgate, bias_ref, wbr, fwd, back, first, cos_t, sin_t, last, perm,
    mixed, turned_a, rows_a,
    send1, recv1, send2, recv2,
    load_sem, s1_sem, r1_sem, s2_sem, r2_sem,
):
    me = lax.axis_index("row") * n_col + lax.axis_index("col")
    chip, core, owners = me // 2, me % 2, n // 2
    local_len, width = tok.shape
    half_len = local_len // 2

    pairs = (
        (wmix_hbm.at[:, pl.ds(0, SPAN)], wmix.at[0]),
        (tok_hbm.at[pl.ds(0, half_len)], tok.at[pl.ds(0, half_len)]),
        (tok_hbm.at[pl.ds(half_len, half_len)], tok.at[pl.ds(half_len, half_len)]),
        (fwd_hbm, fwd), (wmix_hbm.at[:, pl.ds(SPAN, SPAN)], wmix.at[1]),
        (bias_hbm, bias_ref), (wgate_hbm, wgate),
        (first_hbm, first), (cos_hbm, cos_t), (sin_hbm, sin_t), (last_hbm, last),
        (wbr_hbm, wbr), (back_hbm, back), (perm_hbm, perm),
    )
    loads = [pltpu.make_async_copy(a, b, load_sem.at[i]) for i, (a, b) in enumerate(pairs)]
    for i in range(5):
        loads[i].start()

    barrier = pltpu.get_barrier_semaphore()

    def greet(r, carry):
        peer = (me + r) % n
        pl.semaphore_signal(barrier, inc=1, device_id=(peer // n_col, peer % n_col), device_id_type=MESH)
        return carry

    lax.fori_loop(1, n, greet, 0)

    def device(dev):
        return (dev // n_col, dev % n_col)

    def to_owner(h, i):
        return pltpu.make_async_remote_copy(
            src_ref=send1.at[h, i], dst_ref=recv1.at[me],
            send_sem=s1_sem.at[h, i], recv_sem=r1_sem.at[me],
            device_id=device(2 * i + h), device_id_type=MESH,
        )

    def from_source(dev):
        return pltpu.make_async_remote_copy(
            src_ref=send1.at[0, 0], dst_ref=recv1.at[dev],
            send_sem=s1_sem.at[0, 0], recv_sem=r1_sem.at[dev],
            device_id=device(dev), device_id_type=MESH,
        )

    def to_reader(dev):
        return pltpu.make_async_remote_copy(
            src_ref=send2.at[dev], dst_ref=recv2.at[core, chip],
            send_sem=s2_sem.at[dev], recv_sem=r2_sem.at[core, chip],
            device_id=device(dev), device_id_type=MESH,
        )

    def from_owner(h, i):
        return pltpu.make_async_remote_copy(
            src_ref=send2.at[0], dst_ref=recv2.at[h, i],
            send_sem=s2_sem.at[0], recv_sem=r2_sem.at[h, i],
            device_id=device(2 * i + h), device_id_type=MESH,
        )

    def each_owner(h, act):
        def step(r, carry):
            i = chip ^ ((r + 8) % owners)

            @pl.when(2 * i + h != me)
            def _():
                act(h, i)

            return carry

        lax.fori_loop(0, owners, step, 0)

    def each_peer(act):
        def step(r, carry):
            act((me + r) % n)
            return carry

        lax.fori_loop(1, n, step, 0)

    def pack(h):
        packed = dot_t(fwd[...], mixed[:, SPAN * h : SPAN * (h + 1)])
        send1[h] = packed.reshape(owners, UNIT, local_len).astype(jnp.bfloat16)

    loads[0].wait()
    for i in range(2):
        at = slice(half_len * i, half_len * (i + 1))
        loads[1 + i].wait()
        mixed[at, :SPAN] = dot(tok[at, :], wmix[0]).astype(jnp.bfloat16)
    loads[3].wait()
    pack(0)
    pl.semaphore_wait(barrier, n - 1)
    each_owner(0, lambda h, i: to_owner(h, i).start())

    for i in range(5, len(loads)):
        loads[i].start()
    loads[4].wait()
    for i in range(2):
        at = slice(half_len * i, half_len * (i + 1))
        mixed[at, SPAN:] = dot(tok[at, :], wmix[1]).astype(jnp.bfloat16)
    pack(1)
    recv1[me] = send1[core, chip]

    loads[5].wait()
    loads[6].wait()

    def open_gate(i, carry):
        at = pl.ds(pl.multiple_of(i * SPAN, SPAN), SPAN)
        gate[:, at] = jax.nn.sigmoid(dot(tok[...], wgate[:, at]) + bias_ref[:, at])
        return carry

    lax.fori_loop(0, 3, open_gate, 0)
    each_owner(1, lambda h, i: to_owner(h, i).start())
    early = jnp.where(core == 0, 4, width // SPAN)
    lax.fori_loop(3, early, open_gate, 0)
    for i in range(7, len(loads)):
        loads[i].wait()

    def turn(h, out):
        def step(j, carry):
            lanes = pl.ds(pl.multiple_of(j * SPAN, SPAN), SPAN)
            out[:, lanes] = dot(back[...], wbr[SPAN * h : SPAN * (h + 1), lanes]).astype(jnp.bfloat16)
            return carry

        lax.fori_loop(0, width // SPAN, step, 0)

    chunk = n * ROWS
    per = BLOCK // UNIT
    blocks = n // per
    column = core * SPAN + chip * UNIT + lax.broadcasted_iota(jnp.int32, (1, UNIT, local_len), 1)
    is_sin = column % GROUP_DIM > HALF
    c = jnp.broadcast_to(cos_t[...].reshape(n, 1, local_len), (n, ROWS, local_len))
    s = jnp.broadcast_to(sin_t[...].reshape(n, 1, local_len), (n, ROWS, local_len))

    each_peer(lambda peer: from_source(peer).wait_recv())
    for half in range(2):
        at = slice(ROWS * half, ROWS * (half + 1))
        gathered = recv1[...].astype(jnp.float32)[:, at, :].reshape(chunk, local_len).astype(jnp.bfloat16)
        first_re = dot(first[:chunk, :], gathered).reshape(n, ROWS, local_len)
        first_im = dot(first[chunk:, :], gathered).reshape(n, ROWS, local_len)
        turn_c, turn_s = jnp.where(is_sin[:, at, :], s, c), jnp.where(is_sin[:, at, :], -c, s)
        part_re = (first_re * turn_c + first_im * turn_s).reshape(chunk, local_len).astype(jnp.bfloat16)
        part_im = (first_im * turn_c - first_re * turn_s).reshape(chunk, local_len).astype(jnp.bfloat16)
        real = (dot(part_re, last[:local_len, :]) + dot(part_im, last[local_len:, :])) * scale
        for a in range(blocks):
            for b in range(blocks):
                block = real[ROWS * per * a : ROWS * per * (a + 1), BLOCK * b : BLOCK * (b + 1)]
                for i, unit in enumerate(swap_units(block)):
                    send2[per * b + i, at, BLOCK * a : BLOCK * (a + 1)] = unit.astype(jnp.bfloat16)
    each_peer(lambda peer: to_reader(peer).start())
    recv2[core, chip] = send2[me]
    lax.fori_loop(early, width // SPAN, open_gate, 0)
    turn(0, turned_a)
    turn(1, turned_b)

    def rows(h):
        each_owner(h, lambda h, i: from_owner(h, i).wait_recv())
        return dot_t(perm[...], recv2[h].reshape(SPAN, local_len)).astype(jnp.bfloat16)

    each_owner(0, lambda h, i: to_owner(h, i).wait_send())
    each_owner(1, lambda h, i: to_owner(h, i).wait_send())
    rows_a[...] = rows(0)

    def first_half(j, carry):
        lanes = pl.ds(pl.multiple_of(j * SPAN, SPAN), SPAN)
        partial[:, lanes] = gate[:, lanes] * dot(rows_a[...], turned_a[:, lanes])
        return carry

    lax.fori_loop(0, width // SPAN, first_half, 0)
    each_peer(lambda peer: to_reader(peer).wait_send())
    rows_b[...] = rows(1)


def fused(tokens, w_mix, w_gate, gate_bias, w_branch):
    axes = ("row", "col")
    n_dev = lax.axis_size(axes)
    n_col = lax.axis_size("col")
    local_len, width = tokens.shape
    channels = w_mix.shape[1]
    full_len = local_len * n_dev
    bf16, f32 = jnp.bfloat16, jnp.float32

    dev, pos = np.arange(n_dev), np.arange(local_len)
    forward, back = channel_tables(SPAN)
    cos_p, sin_p = phases(dev, dev, n_dev)
    unit = np.eye(ROWS)
    first = np.concatenate([np.kron(cos_p, unit), np.kron(-sin_p, unit)]).astype(bf16)
    cos_t, sin_t = (t.astype(np.float32) for t in phases(dev, pos, full_len))
    last = np.concatenate(phases(pos, pos, local_len)).astype(bf16)
    order = (pos % n_dev) * UNIT + pos // n_dev
    perm = np.eye(local_len)[order].astype(bf16)

    tables = [forward, back, first, cos_t, sin_t, last, perm]
    any_space = pl.BlockSpec(memory_space=pl.ANY)
    by_owner = pltpu.VMEM((2, n_dev // 2, UNIT, local_len), bf16)
    by_device = pltpu.VMEM((n_dev, UNIT, local_len), bf16)
    owner_sems = pltpu.SemaphoreType.DMA((2, n_dev // 2))
    device_sems = pltpu.SemaphoreType.DMA((n_dev,))
    vmem = lambda array: pltpu.VMEM(array.shape, array.dtype)
    gate, partial, turned, rows = pl.pallas_call(
        functools.partial(kernel, n_dev, n_col, 1.0 / math.sqrt(full_len * GROUP_DIM)),
        out_shape=[
            pltpu.VMEM((local_len, width), f32),
            pltpu.VMEM((local_len, width), f32),
            pltpu.VMEM((SPAN, width), bf16),
            pltpu.VMEM((local_len, SPAN), bf16),
        ],
        in_specs=[any_space] * 12,
        out_specs=[pl.BlockSpec(memory_space=pltpu.VMEM)] * 4,
        scratch_shapes=[
            vmem(tokens), pltpu.VMEM((2, width, SPAN), bf16), vmem(w_gate), pltpu.VMEM((1, width), f32), vmem(w_branch),
            vmem(forward), vmem(back), vmem(first), vmem(cos_t), vmem(sin_t), vmem(last), vmem(perm),
            pltpu.VMEM((local_len, channels), bf16),
            pltpu.VMEM((SPAN, width), bf16),
            pltpu.VMEM((local_len, SPAN), bf16),
            by_owner, by_device, by_device, by_owner,
            pltpu.SemaphoreType.DMA((14,)),
            owner_sems, device_sems, device_sems, owner_sems,
        ],
        compiler_params=pltpu.CompilerParams(
            collective_id=0, has_side_effects=True, vmem_limit_bytes=57_200_000
        ),
    )(tokens, w_mix, w_gate, gate_bias.reshape(1, width), w_branch, *[jnp.asarray(t) for t in tables])
    return (partial + gate * dot(rows, turned)).astype(bf16)


def shards(tokens, w_mix, w_gate, gate_bias, w_branch):
    n_dev = lax.axis_size(("row", "col"))
    local_len, channels = tokens.shape[0], w_mix.shape[1]
    tiled = n_dev * ROWS == SPAN and channels == 2 * SPAN and local_len == n_dev * UNIT
    step = fused if tiled else plain
    return step(tokens, w_mix, w_gate, gate_bias, w_branch)


def solution(mesh):
    in_specs = (P(("row", "col"), None), P(), P(), P(), P())
    out_specs = P(("row", "col"), None)
    return jax.shard_map(shards, mesh=mesh, in_specs=in_specs, out_specs=out_specs, check_vma=False)
```

```python
import functools
import math

import jax
import jax.numpy as jnp
import numpy as np
from jax import lax
from jax.experimental import pallas as pl
from jax.experimental.pallas import tpu as pltpu
from jax.sharding import PartitionSpec as P

GROUP_DIM = 64
HALF = GROUP_DIM // 2
UNIT = 16
ROWS = 8
BLOCK = 128
SPAN = 256
FINISH = 8 * 1024 * 1024
MESH = pl.DeviceIdType.MESH


def phases(left, right, period):
    angle = (left[:, None] * right[None, :] % period) * (2.0 * math.pi / period)
    return np.cos(angle), np.sin(angle)


def channel_tables(span):
    index = np.arange(GROUP_DIM)
    packed = np.where(index <= HALF, index, index - HALF)
    cos_c, sin_c = phases(packed, index, GROUP_DIM)
    is_sin = index > HALF
    forward = np.where(is_sin[:, None], sin_c, cos_c)
    back = np.zeros((GROUP_DIM, GROUP_DIM))
    for row in index:
        freq = packed[row]
        mirror = (GROUP_DIM - freq) % GROUP_DIM
        back[row, freq] += -1.0 if is_sin[row] else 1.0
        if mirror != freq:
            back[row, mirror] += 1.0
    copies = np.eye(span // GROUP_DIM)
    return np.kron(copies, forward).astype(jnp.bfloat16), np.kron(copies, back).astype(jnp.bfloat16)


def plain(tokens, w_mix, w_gate, gate_bias, w_branch):
    axes = ("row", "col")
    n_dev = lax.axis_size(axes)
    local_len, full_len = tokens.shape[0], tokens.shape[0] * n_dev
    sub_len = local_len // n_dev
    channels = w_mix.shape[1]
    cols = channels // n_dev
    forward, back = channel_tables(channels)
    mixed_in = jnp.dot(tokens, w_mix, preferred_element_type=jnp.float32).astype(jnp.bfloat16)
    packed = jnp.einsum("ab,nb->an", forward, mixed_in, preferred_element_type=jnp.float32)
    packed = packed.astype(jnp.bfloat16).reshape(n_dev, cols, local_len)
    packed = lax.all_to_all(packed, axes, split_axis=0, concat_axis=0, tiled=True)
    dev, pos = np.arange(n_dev), np.arange(local_len)
    cos_p, sin_p = (t.astype(jnp.bfloat16) for t in phases(dev, dev, n_dev))
    cos_t, sin_t = (jnp.asarray(t, jnp.float32)[:, None, :] for t in phases(dev, pos, full_len))
    cos_m, sin_m = (t.astype(jnp.bfloat16) for t in phases(pos, pos, local_len))
    first_re = jnp.einsum("kp,pcj->kcj", cos_p, packed, preferred_element_type=jnp.float32)
    first_im = -jnp.einsum("kp,pcj->kcj", sin_p, packed, preferred_element_type=jnp.float32)
    column = lax.axis_index(axes) * cols + jnp.arange(cols, dtype=jnp.int32)
    is_sin = (column % GROUP_DIM > HALF)[None, :, None]
    rot_c, rot_s = jnp.where(is_sin, sin_t, cos_t), jnp.where(is_sin, -cos_t, sin_t)
    part_re = (first_re * rot_c + first_im * rot_s).astype(jnp.bfloat16)
    part_im = (first_im * rot_c - first_re * rot_s).astype(jnp.bfloat16)
    real = jnp.einsum("kcj,jm->kcm", part_re, cos_m, preferred_element_type=jnp.float32)
    real = real + jnp.einsum("kcj,jm->kcm", part_im, sin_m, preferred_element_type=jnp.float32)
    real = (real * (1.0 / math.sqrt(full_len * GROUP_DIM))).astype(jnp.bfloat16)
    real = real.reshape(n_dev, cols, n_dev, sub_len).transpose(2, 1, 0, 3)
    real = lax.all_to_all(real, axes, split_axis=0, concat_axis=0, tiled=True)
    rows = real.transpose(3, 2, 0, 1).reshape(local_len, channels)
    turned = jnp.dot(back, w_branch, preferred_element_type=jnp.float32).astype(jnp.bfloat16)
    gate = jax.nn.sigmoid(jnp.dot(tokens, w_gate, preferred_element_type=jnp.float32) + gate_bias)
    return (gate * jnp.dot(rows, turned, preferred_element_type=jnp.float32)).astype(jnp.bfloat16)


def dot(a, b):
    return jnp.dot(a, b, preferred_element_type=jnp.float32)


def dot_t(a, b):
    return lax.dot_general(a, b, (((1,), (1,)), ((), ())), preferred_element_type=jnp.float32)


def swap_units(block):
    units = [block[ROWS * i : ROWS * (i + 1)] for i in range(BLOCK // UNIT)]
    lane = lax.broadcasted_iota(jnp.int32, (ROWS, BLOCK), 1) // UNIT
    for bit in range(3):
        step = 1 << bit
        low = (lane // step) % 2 == 0
        for i in range(len(units)):
            if i & step:
                continue
            a, b = units[i], units[i + step]
            units[i] = jnp.where(low, a, pltpu.roll(b, UNIT * step, 1))
            units[i + step] = jnp.where(low, pltpu.roll(a, BLOCK - UNIT * step, 1), b)
    return units


def kernel(
    n, n_col, scale,
    tok_hbm, wmix_hbm, wgate_hbm, bias_hbm, wbr_hbm,
    fwd_hbm, back_hbm, first_hbm, cos_hbm, sin_hbm, last_hbm, perm_hbm,
    gate, partial, turned_a, turned_b, rows_a, rows_b,
    tok, wmix, wgate, bias_ref, wbr, fwd, back, first, cos_t, sin_t, last, perm,
    mixed,
    send1, recv1, send2, recv2,
    load_sem, s1_sem, r1_sem, s2_sem, r2_sem,
):
    me = lax.axis_index("row") * n_col + lax.axis_index("col")
    chip, core, owners = me // 2, me % 2, n // 2
    local_len, width = tok.shape
    half_len = local_len // 2

    pairs = (
        (wmix_hbm.at[:, pl.ds(0, SPAN)], wmix.at[0]),
        (tok_hbm.at[pl.ds(0, half_len)], tok.at[pl.ds(0, half_len)]),
        (tok_hbm.at[pl.ds(half_len, half_len)], tok.at[pl.ds(half_len, half_len)]),
        (fwd_hbm, fwd), (wmix_hbm.at[:, pl.ds(SPAN, SPAN)], wmix.at[1]),
        (bias_hbm, bias_ref), (wgate_hbm, wgate),
        (first_hbm, first), (cos_hbm, cos_t), (sin_hbm, sin_t), (last_hbm, last),
        (wbr_hbm, wbr), (back_hbm, back), (perm_hbm, perm),
    )
    loads = [pltpu.make_async_copy(a, b, load_sem.at[i]) for i, (a, b) in enumerate(pairs)]
    for i in range(4):
        loads[i].start()

    barrier = pltpu.get_barrier_semaphore()

    def greet(r, carry):
        peer = (me + r) % n
        pl.semaphore_signal(barrier, inc=1, device_id=(peer // n_col, peer % n_col), device_id_type=MESH)
        return carry

    lax.fori_loop(1, n, greet, 0)

    def device(dev):
        return (dev // n_col, dev % n_col)

    def to_owner(h, i):
        return pltpu.make_async_remote_copy(
            src_ref=send1.at[h, i], dst_ref=recv1.at[me],
            send_sem=s1_sem.at[h, i], recv_sem=r1_sem.at[me],
            device_id=device(2 * i + h), device_id_type=MESH,
        )

    def from_source(dev):
        return pltpu.make_async_remote_copy(
            src_ref=send1.at[0, 0], dst_ref=recv1.at[dev],
            send_sem=s1_sem.at[0, 0], recv_sem=r1_sem.at[dev],
            device_id=device(dev), device_id_type=MESH,
        )

    def to_reader(dev):
        return pltpu.make_async_remote_copy(
            src_ref=send2.at[dev], dst_ref=recv2.at[core, chip],
            send_sem=s2_sem.at[dev], recv_sem=r2_sem.at[core, chip],
            device_id=device(dev), device_id_type=MESH,
        )

    def from_owner(h, i):
        return pltpu.make_async_remote_copy(
            src_ref=send2.at[0], dst_ref=recv2.at[h, i],
            send_sem=s2_sem.at[0], recv_sem=r2_sem.at[h, i],
            device_id=device(2 * i + h), device_id_type=MESH,
        )

    def each_owner(h, act):
        def step(r, carry):
            i = chip ^ ((r + 3 * owners // 4) % owners)

            @pl.when(2 * i + h != me)
            def _():
                act(h, i)

            return carry

        lax.fori_loop(0, owners, step, 0)

    def each_peer(act):
        def step(r, carry):
            act((me + r) % n)
            return carry

        lax.fori_loop(1, n, step, 0)

    def pack(h):
        packed = dot_t(fwd[...], mixed[:, SPAN * h : SPAN * (h + 1)])
        send1[h] = packed.reshape(owners, UNIT, local_len).astype(jnp.bfloat16)

    loads[0].wait()
    for i in range(2):
        at = slice(half_len * i, half_len * (i + 1))
        loads[1 + i].wait()
        mixed[at, :SPAN] = dot(tok[at, :], wmix[0]).astype(jnp.bfloat16)
    loads[4].start()
    loads[3].wait()
    pack(0)
    pl.semaphore_wait(barrier, n - 1)
    each_owner(0, lambda h, i: to_owner(h, i).start())

    for i in range(5, len(loads)):
        loads[i].start()
    loads[4].wait()
    for i in range(2):
        at = slice(half_len * i, half_len * (i + 1))
        mixed[at, SPAN:] = dot(tok[at, :], wmix[1]).astype(jnp.bfloat16)
    pack(1)
    recv1[me] = send1[core, chip]

    loads[5].wait()
    loads[6].wait()

    def open_gate(i, carry):
        at = pl.ds(pl.multiple_of(i * SPAN, SPAN), SPAN)
        gate[:, at] = jax.nn.sigmoid(dot(tok[...], wgate[:, at]) + bias_ref[:, at])
        return carry

    lax.fori_loop(0, 2, open_gate, 0)
    each_owner(1, lambda h, i: to_owner(h, i).start())
    early = jnp.where(core == 0, 3, width // SPAN)
    lax.fori_loop(2, early, open_gate, 0)
    for i in range(7, len(loads)):
        loads[i].wait()

    def turn(h, out):
        def step(j, carry):
            lanes = pl.ds(pl.multiple_of(j * SPAN, SPAN), SPAN)
            out[:, lanes] = dot(back[...], wbr[SPAN * h : SPAN * (h + 1), lanes]).astype(jnp.bfloat16)
            return carry

        lax.fori_loop(0, width // SPAN, step, 0)

    chunk = n * ROWS
    per = BLOCK // UNIT
    blocks = n // per
    column = core * SPAN + chip * UNIT + lax.broadcasted_iota(jnp.int32, (1, UNIT, local_len), 1)
    is_sin = column % GROUP_DIM > HALF
    c = jnp.broadcast_to(cos_t[...].reshape(n, 1, local_len), (n, ROWS, local_len))
    s = jnp.broadcast_to(sin_t[...].reshape(n, 1, local_len), (n, ROWS, local_len))

    each_peer(lambda peer: from_source(peer).wait_recv())
    for half in range(2):
        at = slice(ROWS * half, ROWS * (half + 1))
        gathered = recv1[...].astype(jnp.float32)[:, at, :].reshape(chunk, local_len).astype(jnp.bfloat16)
        first_re = dot(first[:chunk, :], gathered).reshape(n, ROWS, local_len)
        first_im = dot(first[chunk:, :], gathered).reshape(n, ROWS, local_len)
        turn_c, turn_s = jnp.where(is_sin[:, at, :], s, c), jnp.where(is_sin[:, at, :], -c, s)
        part_re = (first_re * turn_c + first_im * turn_s).reshape(chunk, local_len).astype(jnp.bfloat16)
        part_im = (first_im * turn_c - first_re * turn_s).reshape(chunk, local_len).astype(jnp.bfloat16)
        real = (dot(part_re, last[:local_len, :]) + dot(part_im, last[local_len:, :])) * scale
        for a in range(blocks):
            for b in range(blocks):
                block = real[ROWS * per * a : ROWS * per * (a + 1), BLOCK * b : BLOCK * (b + 1)]
                for i, unit in enumerate(swap_units(block)):
                    send2[per * b + i, at, BLOCK * a : BLOCK * (a + 1)] = unit.astype(jnp.bfloat16)
    each_peer(lambda peer: to_reader(peer).start())
    recv2[core, chip] = send2[me]
    lax.fori_loop(early, width // SPAN, open_gate, 0)
    turn(0, turned_a)
    turn(1, turned_b)

    def rows(h):
        each_owner(h, lambda h, i: from_owner(h, i).wait_recv())
        return dot_t(perm[...], recv2[h].reshape(SPAN, local_len)).astype(jnp.bfloat16)

    each_owner(0, lambda h, i: to_owner(h, i).wait_send())
    each_owner(1, lambda h, i: to_owner(h, i).wait_send())
    rows_a[...] = rows(0)

    for j in range(8):
        at = slice(SPAN * j, SPAN * (j + 1))
        partial[:, at] = dot(rows_a[...], turned_a[:, at])
    each_peer(lambda peer: to_reader(peer).wait_send())
    rows_b[...] = rows(1)


def finish(gate, partial, turned_a, turned_b, rows_a, rows_b, out_hbm, out, sem):
    width = gate.shape[1]
    tile = 2 * SPAN
    copies = []
    for j in range(width // tile):
        at = slice(tile * j, tile * (j + 1))
        first = partial[:, at] if at.stop <= partial.shape[1] else dot(rows_a[...], turned_a[:, at])
        out[j] = (gate[:, at] * (first + dot(rows_b[...], turned_b[:, at]))).astype(jnp.bfloat16)
        copies.append(pltpu.make_async_copy(out.at[j], out_hbm.at[:, pl.ds(tile * j, tile)], sem.at[j]))
        copies[j].start()
    for copy in copies:
        copy.wait()


def fused(tokens, w_mix, w_gate, gate_bias, w_branch):
    axes = ("row", "col")
    n_dev = lax.axis_size(axes)
    n_col = lax.axis_size("col")
    local_len, width = tokens.shape
    channels = w_mix.shape[1]
    full_len = local_len * n_dev
    bf16, f32 = jnp.bfloat16, jnp.float32

    dev, pos = np.arange(n_dev), np.arange(local_len)
    forward, back = channel_tables(SPAN)
    cos_p, sin_p = phases(dev, dev, n_dev)
    unit = np.eye(ROWS)
    first = np.concatenate([np.kron(cos_p, unit), np.kron(-sin_p, unit)]).astype(bf16)
    cos_t, sin_t = (t.astype(np.float32) for t in phases(dev, pos, full_len))
    last = np.concatenate(phases(pos, pos, local_len)).astype(bf16)
    order = (pos % n_dev) * UNIT + pos // n_dev
    perm = np.eye(local_len)[order].astype(bf16)

    tables = [forward, back, first, cos_t, sin_t, last, perm]
    any_space = pl.BlockSpec(memory_space=pl.ANY)
    by_owner = pltpu.VMEM((2, n_dev // 2, UNIT, local_len), bf16)
    by_device = pltpu.VMEM((n_dev, UNIT, local_len), bf16)
    owner_sems = pltpu.SemaphoreType.DMA((2, n_dev // 2))
    device_sems = pltpu.SemaphoreType.DMA((n_dev,))
    vmem = lambda array: pltpu.VMEM(array.shape, array.dtype)
    outs = pl.pallas_call(
        functools.partial(kernel, n_dev, n_col, 1.0 / math.sqrt(full_len * GROUP_DIM)),
        out_shape=[
            pltpu.VMEM((local_len, width), f32),
            pltpu.VMEM((local_len, SPAN * 8), f32),
            pltpu.VMEM((SPAN, width), bf16),
            pltpu.VMEM((SPAN, width), bf16),
            pltpu.VMEM((local_len, SPAN), bf16),
            pltpu.VMEM((local_len, SPAN), bf16),
        ],
        in_specs=[any_space] * 12,
        out_specs=[pl.BlockSpec(memory_space=pltpu.VMEM)] * 6,
        scratch_shapes=[
            vmem(tokens), pltpu.VMEM((2, width, SPAN), bf16), vmem(w_gate), pltpu.VMEM((1, width), f32), vmem(w_branch),
            vmem(forward), vmem(back), vmem(first), vmem(cos_t), vmem(sin_t), vmem(last), vmem(perm),
            pltpu.VMEM((local_len, channels), bf16),
            by_owner, by_device, by_device, by_owner,
            pltpu.SemaphoreType.DMA((14,)),
            owner_sems, device_sems, device_sems, owner_sems,
        ],
        compiler_params=pltpu.CompilerParams(
            collective_id=0, has_side_effects=True, vmem_limit_bytes=55633280
        ),
    )(tokens, w_mix, w_gate, gate_bias.reshape(1, width), w_branch, *[jnp.asarray(t) for t in tables])
    tiles = width // (2 * SPAN)
    return pl.pallas_call(
        finish,
        out_shape=jax.ShapeDtypeStruct((local_len, width), bf16),
        in_specs=[pl.BlockSpec(memory_space=pltpu.VMEM)] * 6,
        out_specs=any_space,
        scratch_shapes=[pltpu.VMEM((tiles, local_len, 2 * SPAN), bf16), pltpu.SemaphoreType.DMA((tiles,))],
        compiler_params=pltpu.CompilerParams(vmem_limit_bytes=FINISH),
    )(*outs)


def shards(tokens, w_mix, w_gate, gate_bias, w_branch):
    n_dev = lax.axis_size(("row", "col"))
    local_len, channels = tokens.shape[0], w_mix.shape[1]
    tiled = n_dev * ROWS == SPAN and channels == 2 * SPAN and local_len == n_dev * UNIT
    step = fused if tiled else plain
    return step(tokens, w_mix, w_gate, gate_bias, w_branch)


def solution(mesh):
    in_specs = (P(("row", "col"), None), P(), P(), P(), P())
    out_specs = P(("row", "col"), None)
    return jax.shard_map(shards, mesh=mesh, in_specs=in_specs, out_specs=out_specs, check_vma=False)
```

```python
import functools
import math

import jax
import jax.numpy as jnp
import numpy as np
from jax import lax
from jax.experimental import pallas as pl
from jax.experimental.pallas import tpu as pltpu
from jax.sharding import PartitionSpec as P

GROUP_DIM = 64
HALF = GROUP_DIM // 2
UNIT = 16
ROWS = 8
BLOCK = 128
SPAN = 256
FINISH = 8 * 1024 * 1024
MESH = pl.DeviceIdType.MESH


def phases(left, right, period):
    angle = (left[:, None] * right[None, :] % period) * (2.0 * math.pi / period)
    return np.cos(angle), np.sin(angle)


def channel_tables(span):
    index = np.arange(GROUP_DIM)
    packed = np.where(index <= HALF, index, index - HALF)
    cos_c, sin_c = phases(packed, index, GROUP_DIM)
    is_sin = index > HALF
    forward = np.where(is_sin[:, None], sin_c, cos_c)
    back = np.zeros((GROUP_DIM, GROUP_DIM))
    for row in index:
        freq = packed[row]
        mirror = (GROUP_DIM - freq) % GROUP_DIM
        back[row, freq] += -1.0 if is_sin[row] else 1.0
        if mirror != freq:
            back[row, mirror] += 1.0
    copies = np.eye(span // GROUP_DIM)
    return np.kron(copies, forward).astype(jnp.bfloat16), np.kron(copies, back).astype(jnp.bfloat16)


def plain(tokens, w_mix, w_gate, gate_bias, w_branch):
    axes = ("row", "col")
    n_dev = lax.axis_size(axes)
    local_len, full_len = tokens.shape[0], tokens.shape[0] * n_dev
    sub_len = local_len // n_dev
    channels = w_mix.shape[1]
    cols = channels // n_dev
    forward, back = channel_tables(channels)
    mixed_in = jnp.dot(tokens, w_mix, preferred_element_type=jnp.float32).astype(jnp.bfloat16)
    packed = jnp.einsum("ab,nb->an", forward, mixed_in, preferred_element_type=jnp.float32)
    packed = packed.astype(jnp.bfloat16).reshape(n_dev, cols, local_len)
    packed = lax.all_to_all(packed, axes, split_axis=0, concat_axis=0, tiled=True)
    dev, pos = np.arange(n_dev), np.arange(local_len)
    cos_p, sin_p = (t.astype(jnp.bfloat16) for t in phases(dev, dev, n_dev))
    cos_t, sin_t = (jnp.asarray(t, jnp.float32)[:, None, :] for t in phases(dev, pos, full_len))
    cos_m, sin_m = (t.astype(jnp.bfloat16) for t in phases(pos, pos, local_len))
    first_re = jnp.einsum("kp,pcj->kcj", cos_p, packed, preferred_element_type=jnp.float32)
    first_im = -jnp.einsum("kp,pcj->kcj", sin_p, packed, preferred_element_type=jnp.float32)
    column = lax.axis_index(axes) * cols + jnp.arange(cols, dtype=jnp.int32)
    is_sin = (column % GROUP_DIM > HALF)[None, :, None]
    rot_c, rot_s = jnp.where(is_sin, sin_t, cos_t), jnp.where(is_sin, -cos_t, sin_t)
    part_re = (first_re * rot_c + first_im * rot_s).astype(jnp.bfloat16)
    part_im = (first_im * rot_c - first_re * rot_s).astype(jnp.bfloat16)
    real = jnp.einsum("kcj,jm->kcm", part_re, cos_m, preferred_element_type=jnp.float32)
    real = real + jnp.einsum("kcj,jm->kcm", part_im, sin_m, preferred_element_type=jnp.float32)
    real = (real * (1.0 / math.sqrt(full_len * GROUP_DIM))).astype(jnp.bfloat16)
    real = real.reshape(n_dev, cols, n_dev, sub_len).transpose(2, 1, 0, 3)
    real = lax.all_to_all(real, axes, split_axis=0, concat_axis=0, tiled=True)
    rows = real.transpose(3, 2, 0, 1).reshape(local_len, channels)
    turned = jnp.dot(back, w_branch, preferred_element_type=jnp.float32).astype(jnp.bfloat16)
    gate = jax.nn.sigmoid(jnp.dot(tokens, w_gate, preferred_element_type=jnp.float32) + gate_bias)
    return (gate * jnp.dot(rows, turned, preferred_element_type=jnp.float32)).astype(jnp.bfloat16)


def dot(a, b):
    return jnp.dot(a, b, preferred_element_type=jnp.float32)


def dot_t(a, b):
    return lax.dot_general(a, b, (((1,), (1,)), ((), ())), preferred_element_type=jnp.float32)


def swap_units(block):
    units = [block[ROWS * i : ROWS * (i + 1)] for i in range(BLOCK // UNIT)]
    lane = lax.broadcasted_iota(jnp.int32, (ROWS, BLOCK), 1) // UNIT
    for bit in range(3):
        step = 1 << bit
        low = (lane // step) % 2 == 0
        for i in range(len(units)):
            if i & step:
                continue
            a, b = units[i], units[i + step]
            units[i] = jnp.where(low, a, pltpu.roll(b, UNIT * step, 1))
            units[i + step] = jnp.where(low, pltpu.roll(a, BLOCK - UNIT * step, 1), b)
    return units


def kernel(
    n, n_col, scale,
    tok_hbm, wmix_hbm, wgate_hbm, bias_hbm, wbr_hbm,
    fwd_hbm, back_hbm, first_hbm, cos_hbm, sin_hbm, last_hbm, perm_hbm,
    gate, partial, turned_a, turned_b, rows_a, rows_b,
    tok, wmix, wgate, bias_ref, wbr, fwd, back, first, cos_t, sin_t, last, perm,
    mixed,
    send1, recv1, send2, recv2,
    load_sem, s1_sem, r1_sem, s2_sem, r2_sem,
):
    me = lax.axis_index("row") * n_col + lax.axis_index("col")
    chip, core, owners = me // 2, me % 2, n // 2
    local_len, width = tok.shape
    half_len = local_len // 2

    pairs = (
        (wmix_hbm.at[:, pl.ds(0, SPAN)], wmix.at[0]),
        (tok_hbm.at[pl.ds(0, half_len)], tok.at[pl.ds(0, half_len)]),
        (tok_hbm.at[pl.ds(half_len, half_len)], tok.at[pl.ds(half_len, half_len)]),
        (fwd_hbm, fwd), (wmix_hbm.at[:, pl.ds(SPAN, SPAN)], wmix.at[1]),
        (bias_hbm, bias_ref), (wgate_hbm, wgate),
        (first_hbm, first), (cos_hbm, cos_t), (sin_hbm, sin_t), (last_hbm, last),
        (wbr_hbm, wbr), (back_hbm, back), (perm_hbm, perm),
    )
    loads = [pltpu.make_async_copy(a, b, load_sem.at[i]) for i, (a, b) in enumerate(pairs)]
    for i in range(4):
        loads[i].start()

    barrier = pltpu.get_barrier_semaphore()

    def greet(r, carry):
        peer = (me + r) % n
        pl.semaphore_signal(barrier, inc=1, device_id=(peer // n_col, peer % n_col), device_id_type=MESH)
        return carry

    for r in range(1, n):
        greet(r, 0)

    def device(dev):
        return (dev // n_col, dev % n_col)

    def to_owner(h, i):
        return pltpu.make_async_remote_copy(
            src_ref=send1.at[h, i], dst_ref=recv1.at[me],
            send_sem=s1_sem.at[h, i], recv_sem=r1_sem.at[me],
            device_id=device(2 * i + h), device_id_type=MESH,
        )

    def from_source(dev):
        return pltpu.make_async_remote_copy(
            src_ref=send1.at[0, 0], dst_ref=recv1.at[dev],
            send_sem=s1_sem.at[0, 0], recv_sem=r1_sem.at[dev],
            device_id=device(dev), device_id_type=MESH,
        )

    def to_reader(dev):
        return pltpu.make_async_remote_copy(
            src_ref=send2.at[dev], dst_ref=recv2.at[core, chip],
            send_sem=s2_sem.at[dev], recv_sem=r2_sem.at[core, chip],
            device_id=device(dev), device_id_type=MESH,
        )

    def from_owner(h, i):
        return pltpu.make_async_remote_copy(
            src_ref=send2.at[0], dst_ref=recv2.at[h, i],
            send_sem=s2_sem.at[0], recv_sem=r2_sem.at[h, i],
            device_id=device(2 * i + h), device_id_type=MESH,
        )

    def each_owner(h, act):
        def step(r, carry):
            i = chip ^ ((r + (3 - 3 * h) * owners // 4) % owners)

            @pl.when(2 * i + h != me)
            def _():
                act(h, i)

            return carry

        lax.fori_loop(0, owners, step, 0)

    def each_peer(act):
        def step(r, carry):
            act((me + r) % n)
            return carry

        lax.fori_loop(1, n, step, 0)

    def pack(h):
        packed = dot_t(fwd[...], mixed[:, SPAN * h : SPAN * (h + 1)])
        send1[h] = packed.reshape(owners, UNIT, local_len).astype(jnp.bfloat16)

    loads[0].wait()
    for i in range(2):
        at = slice(half_len * i, half_len * (i + 1))
        loads[1 + i].wait()
        mixed[at, :SPAN] = dot(tok[at, :], wmix[0]).astype(jnp.bfloat16)
    loads[4].start()
    loads[3].wait()
    pack(0)
    pl.semaphore_wait(barrier, n - 1)
    each_owner(0, lambda h, i: to_owner(h, i).start())

    for i in range(5, len(loads)):
        loads[i].start()
    loads[4].wait()
    for i in range(2):
        at = slice(half_len * i, half_len * (i + 1))
        mixed[at, SPAN:] = dot(tok[at, :], wmix[1]).astype(jnp.bfloat16)
    pack(1)
    recv1[me] = send1[core, chip]

    loads[5].wait()
    loads[6].wait()

    def open_gate(i, carry):
        at = pl.ds(pl.multiple_of(i * SPAN, SPAN), SPAN)
        gate[:, at] = jax.nn.sigmoid(dot(tok[...], wgate[:, at]) + bias_ref[:, at])
        return carry

    lax.fori_loop(0, 2, open_gate, 0)
    each_owner(1, lambda h, i: to_owner(h, i).start())
    early = jnp.where(core == 0, 3, width // SPAN)
    lax.fori_loop(2, early, open_gate, 0)
    for i in range(7, len(loads)):
        loads[i].wait()

    def turn(h, out):
        def step(j, carry):
            lanes = pl.ds(pl.multiple_of(j * SPAN, SPAN), SPAN)
            out[:, lanes] = dot(back[...], wbr[SPAN * h : SPAN * (h + 1), lanes]).astype(jnp.bfloat16)
            return carry

        lax.fori_loop(0, width // SPAN, step, 0)

    chunk = n * ROWS
    per = BLOCK // UNIT
    blocks = n // per
    column = core * SPAN + chip * UNIT + lax.broadcasted_iota(jnp.int32, (1, UNIT, local_len), 1)
    is_sin = column % GROUP_DIM > HALF
    c = jnp.broadcast_to(cos_t[...].reshape(n, 1, local_len), (n, ROWS, local_len))
    s = jnp.broadcast_to(sin_t[...].reshape(n, 1, local_len), (n, ROWS, local_len))

    each_peer(lambda peer: from_source(peer).wait_recv())
    for half in range(2):
        at = slice(ROWS * half, ROWS * (half + 1))
        gathered = recv1[...].astype(jnp.float32)[:, at, :].reshape(chunk, local_len).astype(jnp.bfloat16)
        first_re = dot(first[:chunk, :], gathered).reshape(n, ROWS, local_len)
        first_im = dot(first[chunk:, :], gathered).reshape(n, ROWS, local_len)
        turn_c, turn_s = jnp.where(is_sin[:, at, :], s, c), jnp.where(is_sin[:, at, :], -c, s)
        part_re = (first_re * turn_c + first_im * turn_s).reshape(chunk, local_len).astype(jnp.bfloat16)
        part_im = (first_im * turn_c - first_re * turn_s).reshape(chunk, local_len).astype(jnp.bfloat16)
        real = (dot(part_re, last[:local_len, :]) + dot(part_im, last[local_len:, :])) * scale
        for a in range(blocks):
            for b in range(blocks):
                block = real[ROWS * per * a : ROWS * per * (a + 1), BLOCK * b : BLOCK * (b + 1)]
                for i, unit in enumerate(swap_units(block)):
                    send2[per * b + i, at, BLOCK * a : BLOCK * (a + 1)] = unit.astype(jnp.bfloat16)
    each_peer(lambda peer: to_reader(peer).start())
    recv2[core, chip] = send2[me]
    lax.fori_loop(early, width // SPAN, open_gate, 0)
    turn(0, turned_a)
    turn(1, turned_b)

    def rows(h):
        each_owner(h, lambda h, i: from_owner(h, i).wait_recv())
        return dot_t(perm[...], recv2[h].reshape(SPAN, local_len)).astype(jnp.bfloat16)

    each_owner(0, lambda h, i: to_owner(h, i).wait_send())
    each_owner(1, lambda h, i: to_owner(h, i).wait_send())
    rows_a[...] = rows(0)

    for j in range(8):
        at = slice(SPAN * j, SPAN * (j + 1))
        partial[:, at] = dot(rows_a[...], turned_a[:, at])
    each_peer(lambda peer: to_reader(peer).wait_send())
    rows_b[...] = rows(1)


def finish(gate, partial, turned_a, turned_b, rows_a, rows_b, out_hbm, out, sem):
    width = gate.shape[1]
    edges = (0, SPAN, 3 * SPAN, 5 * SPAN, 7 * SPAN, 8 * SPAN)
    copies = []
    for j, (lo, hi) in enumerate(zip(edges, edges[1:])):
        at = slice(lo, hi)
        first = partial[:, at] if at.stop <= partial.shape[1] else dot(rows_a[...], turned_a[:, at])
        out[:, at] = (gate[:, at] * (first + dot(rows_b[...], turned_b[:, at]))).astype(jnp.bfloat16)
        copies.append(pltpu.make_async_copy(out.at[:, at], out_hbm.at[:, at], sem.at[j]))
        copies[j].start()
    for copy in copies:
        copy.wait()


def fused(tokens, w_mix, w_gate, gate_bias, w_branch):
    axes = ("row", "col")
    n_dev = lax.axis_size(axes)
    n_col = lax.axis_size("col")
    local_len, width = tokens.shape
    channels = w_mix.shape[1]
    full_len = local_len * n_dev
    bf16, f32 = jnp.bfloat16, jnp.float32

    dev, pos = np.arange(n_dev), np.arange(local_len)
    forward, back = channel_tables(SPAN)
    cos_p, sin_p = phases(dev, dev, n_dev)
    unit = np.eye(ROWS)
    first = np.concatenate([np.kron(cos_p, unit), np.kron(-sin_p, unit)]).astype(bf16)
    cos_t, sin_t = (t.astype(np.float32) for t in phases(dev, pos, full_len))
    last = np.concatenate(phases(pos, pos, local_len)).astype(bf16)
    order = (pos % n_dev) * UNIT + pos // n_dev
    perm = np.eye(local_len)[order].astype(bf16)

    tables = [forward, back, first, cos_t, sin_t, last, perm]
    any_space = pl.BlockSpec(memory_space=pl.ANY)
    by_owner = pltpu.VMEM((2, n_dev // 2, UNIT, local_len), bf16)
    by_device = pltpu.VMEM((n_dev, UNIT, local_len), bf16)
    owner_sems = pltpu.SemaphoreType.DMA((2, n_dev // 2))
    device_sems = pltpu.SemaphoreType.DMA((n_dev,))
    vmem = lambda array: pltpu.VMEM(array.shape, array.dtype)
    outs = pl.pallas_call(
        functools.partial(kernel, n_dev, n_col, 1.0 / math.sqrt(full_len * GROUP_DIM)),
        out_shape=[
            pltpu.VMEM((local_len, width), f32),
            pltpu.VMEM((local_len, SPAN * 8), f32),
            pltpu.VMEM((SPAN, width), bf16),
            pltpu.VMEM((SPAN, width), bf16),
            pltpu.VMEM((local_len, SPAN), bf16),
            pltpu.VMEM((local_len, SPAN), bf16),
        ],
        in_specs=[any_space] * 12,
        out_specs=[pl.BlockSpec(memory_space=pltpu.VMEM)] * 6,
        scratch_shapes=[
            vmem(tokens), pltpu.VMEM((2, width, SPAN), bf16), vmem(w_gate), pltpu.VMEM((1, width), f32), vmem(w_branch),
            vmem(forward), vmem(back), vmem(first), vmem(cos_t), vmem(sin_t), vmem(last), vmem(perm),
            pltpu.VMEM((local_len, channels), bf16),
            by_owner, by_device, by_device, by_owner,
            pltpu.SemaphoreType.DMA((14,)),
            owner_sems, device_sems, device_sems, owner_sems,
        ],
        compiler_params=pltpu.CompilerParams(
            collective_id=0, has_side_effects=True, vmem_limit_bytes=55633280
        ),
    )(tokens, w_mix, w_gate, gate_bias.reshape(1, width), w_branch, *[jnp.asarray(t) for t in tables])
    return pl.pallas_call(
        finish,
        out_shape=jax.ShapeDtypeStruct((local_len, width), bf16),
        in_specs=[pl.BlockSpec(memory_space=pltpu.VMEM)] * 6,
        out_specs=any_space,
        scratch_shapes=[pltpu.VMEM((local_len, width), bf16), pltpu.SemaphoreType.DMA((5,))],
        compiler_params=pltpu.CompilerParams(vmem_limit_bytes=FINISH),
    )(*outs)


def shards(tokens, w_mix, w_gate, gate_bias, w_branch):
    n_dev = lax.axis_size(("row", "col"))
    local_len, channels = tokens.shape[0], w_mix.shape[1]
    tiled = n_dev * ROWS == SPAN and channels == 2 * SPAN and local_len == n_dev * UNIT
    step = fused if tiled else plain
    return step(tokens, w_mix, w_gate, gate_bias, w_branch)


def solution(mesh):
    in_specs = (P(("row", "col"), None), P(), P(), P(), P())
    out_specs = P(("row", "col"), None)
    return jax.shard_map(shards, mesh=mesh, in_specs=in_specs, out_specs=out_specs, check_vma=False)
```
